128 devices in a mesh: sp: 16 (over z, y), tp: 8 (over x, core).
Axes of the slice: x: 4, y: 4, z: 4, core: 2. Of those that a mesh axis runs over, the one named last changes fastest.
Arguments:
- queries: bfloat16 [16384, 8, 128], P('sp', 'tp'), may hold values from -160 to 160
- keys_values: bfloat16 [16384, 8, 128], P('sp', 'tp'), may hold values from -5 to 5
- sink_logits: float32 [8, 2], P('tp'), may hold values from 2 to 7
- doc_ids: int32 [16384], replicated, may hold values from 0 to 5, never falling along the last dimension, each value on 1 to 4096 neighbouring positions
- residual: bfloat16 [16384, 2048], P('sp'), may hold values from -6 to 6
- out_weight: bfloat16 [1024, 2048], P('tp'), may hold values from -1.5 to 1.5
- ffn_gain: float32 [2048], replicated, may hold values from 0.1 to 1.9
- gate_weight: bfloat16 [2048, 5120], P('sp', 'tp'), may hold values from -0.125 to 0.125
- value_weight: bfloat16 [2048, 5120], P('sp', 'tp'), may hold values from -0.125 to 0.125
- conv_taps: float32 [3, 5120], P(None, 'tp'), may hold values from -4 to 4
- down_weight: bfloat16 [2048, 5120], P('sp', 'tp'), may hold values from -0.078125 to 0.078125
Outputs:
- layer_out: bfloat16 [16384, 2048], P(('sp', 'tp'))
The draws below stay inside these ranges and needn't reach their ends.
Inputs may be any that keep to these rules, and one draw needn't show every extreme that they name: `doc_ids`: document numbers never fall along the sequence; a document spans at most 4096 positions.
All inputs are finite; a program needn't handle non-finite values.
Results may differ from the reference program's by a relative error of at most 0.02.
Values may be sent and summed in bfloat16 or wider, within the bound.
No kernel may reach another device: no remote copies, remote signals or barrier semaphores. Data moves between devices by JAX's collectives and lax.ppermute only.
A program may use at most 128 MiB of HBM per device.

```python
import math
import jax
import jax.numpy as jnp
import numpy as np
from jax import lax

D = 2048
KV_HEADS = 8
GROUP = 2
HEAD_DIM = 64
ATTN = 1024
FF = 5120
WINDOW = 128
TOKENS = 16384
DOCS = 6
DOC_MOST = 4096
N_TP = 8


def drawn_pair(key):
    base = jax.random.fold_in(key, 4099)
    key_query, key_pairs = jax.random.split(base)
    pairs = jnp.clip(jax.random.normal(key_pairs, (TOKENS, KV_HEADS, 2 * HEAD_DIM), jnp.float32), -5.0, 5.0)
    asked = jnp.clip(jax.random.normal(key_query, (TOKENS, KV_HEADS, GROUP * HEAD_DIM), jnp.float32), -5.0, 5.0)
    return (asked, pairs)


def draw_queries(key, part):
    return drawn_pair(key)[0].astype(jnp.bfloat16)


def draw_keys_values(key, part):
    return drawn_pair(key)[1].astype(jnp.bfloat16)


def shard_levels(rng, dims, cuts, smallest, top_value):
    def one(axis_at, parts):
        draws = jax.random.uniform(jax.random.fold_in(jax.random.fold_in(rng, 6), axis_at), (parts,), jnp.float32, smallest / len(cuts), top_value / len(cuts))
        return jnp.repeat(jnp.exp(draws), dims[axis_at] // parts).reshape((-1,) + (1,) * (len(dims) - axis_at - 1))

    gain = one(*cuts[0])
    for cut in cuts[1:]:
        gain = gain * one(*cut)
    return gain


def split_up(count, total, bound, skew):
    loads = [(1 << 20) // math.isqrt(standing ** skew) + 1 for standing in range(2, count + 1)]
    surplus, counts = total - bound - (count - 1), [1] * (count - 1)
    while surplus > 0:
        candidates = [i for i in range(count - 1) if counts[i] < bound]
        mass, remaining = sum([loads[i] for i in candidates]), surplus
        for i in candidates:
            extra = min(bound - counts[i], max(1, remaining * loads[i] // mass), surplus)
            counts[i] = counts[i] + extra
            surplus = surplus - extra
    return np.array([bound] + counts)


def ragged(key, amount, total, bound, slope):
    if amount == 2:
        one = jax.random.randint(key, (), max(1, total - bound), min(bound, total - 1) + 1)
        return jnp.stack([one, total - one])
    tallies = jnp.asarray(split_up(amount, total, bound, slope), jnp.int32)
    pairs = (amount - 1) // 2
    source_of, sink = tallies[1:1 + 2 * pairs:2], tallies[2:2 + 2 * pairs:2]
    slack = jnp.minimum(source_of - 1, bound - sink)
    passed = jax.random.randint(jax.random.fold_in(key, 1), (pairs,), 0, 1 << 20) % (slack + 1)
    tallies = tallies.at[1:1 + 2 * pairs:2].set(source_of - passed).at[2:2 + 2 * pairs:2].set(sink + passed)
    return tallies[jax.random.permutation(jax.random.fold_in(key, 2), amount)]


def bell_draw(rng, extent, spread, limit, shards=(), held_as=jnp.bfloat16):
    factor_of = shard_levels(rng, extent, shards, -0.22, 0.18) if shards else 1.0
    values = jax.random.normal(rng, extent, jnp.float32) * spread * factor_of
    return jnp.minimum(jnp.maximum(values, -limit), limit).astype(held_as)


def setup_inputs(seed: int = 0) -> dict:
    streams_of = jax.random.split(jax.random.key(seed), 12)
    queries = draw_queries(jax.random.fold_in(streams_of[11], 71), 0)
    keys_values = draw_keys_values(jax.random.fold_in(streams_of[11], 71), 0)
    sink_logits = jnp.clip(2.0 + 5.0 * jax.random.uniform(streams_of[2], (KV_HEADS, GROUP), jnp.float32) ** shard_levels(streams_of[2], (KV_HEADS, GROUP), ((0, 8),), -0.2, 0.2), 2.0, 7.0)
    doc_ids = jnp.searchsorted(jnp.cumsum(ragged(streams_of[3], DOCS, TOKENS, DOC_MOST, 0)), jnp.arange(TOKENS), side="right").astype(jnp.int32)
    residual = bell_draw(streams_of[4], (TOKENS, D), 1.0, 6.0, ((0, 16),))
    out_weight = bell_draw(streams_of[5], (ATTN, D), (ATTN // 64) ** -0.5, 1.5, ((0, 8),))
    ffn_gain = jnp.clip(1.0 + 0.18 * jax.random.normal(streams_of[6], (D,), jnp.float32), 0.1, 1.9)
    gate_weight = bell_draw(streams_of[7], (D, FF), D ** -0.5, 0.125, ((0, 16), (1, 8)))
    value_weight = bell_draw(streams_of[8], (D, FF), D ** -0.5, 0.125, ((0, 16), (1, 8)))
    conv_taps = bell_draw(streams_of[9], (3, FF), 1.2, 4.0, ((1, 8),), jnp.float32)
    down_weight = bell_draw(streams_of[10], (D, FF), FF ** -0.5, 0.078125, ((0, 16), (1, 8)))
    return {"queries": queries, "keys_values": keys_values, "sink_logits": sink_logits, "doc_ids": doc_ids, "residual": residual, "out_weight": out_weight, "ffn_gain": ffn_gain, "gate_weight": gate_weight, "value_weight": value_weight, "conv_taps": conv_taps, "down_weight": down_weight}


norm_epsilon = 1e-06
masked_score = -1e+30
contract_last = (((1,), (1,)), ((), ()))

def rounded(values):
    return lax.optimization_barrier(values.astype(jnp.bfloat16)).astype(jnp.float32)

def band_blocks(padded, block_count, window_rows):
    row_block = padded.reshape((block_count + 2, window_rows) + padded.shape[1:])
    return jnp.concatenate([row_block[:-2], row_block[1:-1], row_block[2:]], axis=1)

def reference(queries, keys_values, sink_logits, doc_ids, residual, out_weight, ffn_gain, gate_weight, value_weight, conv_taps, down_weight):
    window_rows = WINDOW
    block_count = TOKENS // window_rows
    padded = jnp.pad(keys_values, ((window_rows, window_rows), (0, 0), (0, 0)))
    blocks = band_blocks(padded, block_count, window_rows)
    padded_docs = jnp.pad(doc_ids, window_rows, constant_values=-1)
    key_docs = band_blocks(padded_docs, block_count, window_rows)
    query_docs = doc_ids.reshape(block_count, window_rows)
    distance = jnp.arange(window_rows)[:, None] + window_rows - jnp.arange(3 * window_rows)[None, :]
    allowed = (jnp.abs(distance) <= WINDOW)[None] & (query_docs[:, :, None] == key_docs[:, None, :])
    query_blocks = queries.reshape(block_count, window_rows, KV_HEADS, GROUP, HEAD_DIM)

    def one_head(head):
        query_part = query_blocks[:, :, head].astype(jnp.float32)
        key_part = blocks[:, :, head, :HEAD_DIM].astype(jnp.float32)
        value_part = blocks[:, :, head, HEAD_DIM:].astype(jnp.float32)
        scores = jnp.einsum('nqgd,nsd->ngqs', query_part, key_part) * HEAD_DIM ** (-0.5)
        scores = jnp.where(allowed[:, None], scores, masked_score)
        sink_part = sink_logits[head].astype(jnp.float32)[None, :, None, None]
        top_score = jnp.maximum(lax.optimization_barrier(jnp.max(scores, axis=-1, keepdims=True)), sink_part)
        exp_scores = jnp.exp(scores - top_score)
        denominator = lax.optimization_barrier(jnp.sum(exp_scores, axis=-1, keepdims=True)) + jnp.exp(sink_part - top_score)
        probs = rounded(exp_scores / denominator)
        result = jnp.einsum('ngqs,nsd->nqgd', probs, value_part)
        return result.reshape(TOKENS, GROUP * HEAD_DIM)
    per_head = lax.map(one_head, jnp.arange(KV_HEADS))
    attended = jnp.transpose(per_head, (1, 0, 2)).reshape(TOKENS, ATTN).astype(jnp.bfloat16)
    share = ATTN // N_TP
    projected = jnp.zeros((TOKENS, D), jnp.float32)
    for shard in range(N_TP):
        partial_value = jnp.dot(attended[:, shard * share:(shard + 1) * share], out_weight[shard * share:(shard + 1) * share], preferred_element_type=jnp.float32)
        projected = projected + rounded(partial_value)
    stream = (residual.astype(jnp.float32) + projected).astype(jnp.bfloat16)
    stream_f = stream.astype(jnp.float32)
    scale = lax.rsqrt(lax.optimization_barrier(jnp.mean(stream_f * stream_f, axis=-1, keepdims=True)) + norm_epsilon)
    normed = (stream_f * scale * ffn_gain).astype(jnp.bfloat16)
    same_doc = (doc_ids[1:] == doc_ids[:-1]).astype(jnp.float32)
    prev_same = jnp.concatenate([jnp.zeros((1,), jnp.float32), same_doc])[:, None]
    next_same = jnp.concatenate([same_doc, jnp.zeros((1,), jnp.float32)])[:, None]
    hidden_share = FF // N_TP
    lowered = jnp.zeros((TOKENS, D), jnp.float32)
    for shard in range(N_TP):
        lo_col = shard * hidden_share
        hi_col = lo_col + hidden_share
        gate_pre = rounded(jnp.dot(normed, gate_weight[:, lo_col:hi_col], preferred_element_type=jnp.float32))
        value_pre = jnp.dot(normed, value_weight[:, lo_col:hi_col], preferred_element_type=jnp.float32)
        taps = conv_taps[:, lo_col:hi_col]
        before = jnp.pad(gate_pre, ((1, 0), (0, 0)))[:-1] * prev_same
        after = jnp.pad(gate_pre, ((0, 1), (0, 0)))[1:] * next_same
        conved = taps[0] * before + taps[1] * gate_pre + taps[2] * after
        hidden = (jax.nn.gelu(conved, approximate=True) * value_pre).astype(jnp.bfloat16)
        partial_value = lax.dot_general(hidden, down_weight[:, lo_col:hi_col], contract_last, preferred_element_type=jnp.float32)
        lowered = lowered + rounded(partial_value)
    return (stream_f + lowered).astype(jnp.bfloat16)
```

```python
import functools

import jax
import jax.numpy as jnp
from jax import lax
from jax.experimental import pallas as pl
from jax.experimental.pallas import tpu as pltpu
from jax.sharding import PartitionSpec as P


WINDOW = 128
HEAD_DIM = 64
HALO = 144
EXTRA = 16
EPSILON = 1e-06
MASKED = -1e30
F32 = jnp.float32
BF16 = jnp.bfloat16
BIG_VMEM = 60 * 1024 * 1024
LAST = (((1,), (1,)), ((), ()))


def grid_shift(x, dz, dy, nz, ny):
    perm = [
        (z * ny + y, ((z + dz) % nz) * ny + (y + dy) % ny) for z in range(nz) for y in range(ny)
    ]
    return lax.ppermute(x, "sp", perm)


def tp_shift(x, dx, swap, nx):
    perm = [
        (i * 2 + c, ((i + dx) % nx) * 2 + (1 - c if swap else c)) for i in range(nx) for c in range(2)
    ]
    return lax.ppermute(x, "tp", perm)


def swap_cores(x):
    return tp_shift(x, 0, True, lax.axis_size("tp") // 2)


def attention_kernel(sink_ref, q_ref, qx_ref, kv_ref, kl_ref, kr_ref, docs_ref, edocs_ref, qdocs_ref, out_ref, kvx):
    rows = q_ref.shape[0]
    width = 2 * HEAD_DIM
    kvx[0:HALO] = kl_ref[...]
    kvx[HALO : HALO + rows] = kv_ref[...]
    kvx[HALO + rows :] = kr_ref[...]

    def heads(q, keys, allowed):
        n = q.shape[0]
        low = lax.broadcasted_iota(jnp.int32, (n, width), 1) < HEAD_DIM
        swapped = jnp.concatenate([q[:, HEAD_DIM:], q[:, :HEAD_DIM]], axis=1)
        zero = jnp.zeros_like(q)
        results = []
        for g, part in enumerate((jnp.where(low, q, zero), jnp.where(low, swapped, zero))):
            scores = lax.dot_general(part, keys, LAST, preferred_element_type=F32) * HEAD_DIM**-0.5
            scores = jnp.where(allowed, scores, MASKED)
            sink = sink_ref[0, g]
            top = jnp.maximum(jnp.max(scores, axis=-1, keepdims=True), sink)
            e = jnp.exp(scores - top)
            total = jnp.sum(e, axis=-1, keepdims=True) + jnp.exp(sink - top)
            probs = (e * (1.0 / total)).astype(BF16)
            results.append(jnp.dot(probs, keys, preferred_element_type=F32))
        first = jnp.concatenate([results[0][:, HEAD_DIM:], results[0][:, :HEAD_DIM]], axis=1)
        return jnp.where(low, first, results[1]).astype(BF16)

    w = WINDOW
    near = (
        jnp.abs(
            lax.broadcasted_iota(jnp.int32, (w, 3 * w), 0)
            + w
            - lax.broadcasted_iota(jnp.int32, (w, 3 * w), 1)
        )
        <= WINDOW
    )
    for i in range(rows // w):
        own = docs_ref[:, w * (i + 1) : w * (i + 2)]
        own_column = jnp.transpose(jnp.broadcast_to(own, (w, w)))
        own_wide = jnp.concatenate([own_column] * 3, axis=1)
        allowed = near & (own_wide == docs_ref[:, w * i : w * (i + 3)])
        start = HALO - w + w * i
        out_ref[w * i : w * (i + 1)] = heads(q_ref[w * i : w * (i + 1)], kvx[start : start + 3 * w], allowed)

    span = 2 * HALO
    keys = jnp.concatenate([kvx[0:span], kvx[rows : rows + span]], axis=0)
    row = lax.broadcasted_iota(jnp.int32, (EXTRA, 2 * span), 0)
    col = lax.broadcasted_iota(jnp.int32, (EXTRA, 2 * span), 1)
    key_at = jnp.where(col < span, col - HALO, col - span + rows - HALO)
    at = jnp.where(row == 0, rows, -1)
    real = (row == 0) | (row == EXTRA - 1)
    allowed = real & (jnp.abs(at - key_at) <= WINDOW) & (qdocs_ref[...] == edocs_ref[...])
    out_ref[rows : rows + EXTRA] = heads(qx_ref[...], keys, allowed)


def attend(q, kv, sink_logits, docs_f, offset, left, right):
    rows = q.shape[0]
    kl, kr = left[:HALO], right[:HALO]
    qx = jnp.concatenate([right[HALO : HALO + 1], jnp.zeros((EXTRA - 2, q.shape[1]), BF16), left[HALO : HALO + 1]], axis=0)
    near = lax.dynamic_slice_in_dim(docs_f, offset, rows + 2 * HALO)[None]
    docs = near[:, HALO - WINDOW : HALO + rows + WINDOW]
    edocs = jnp.concatenate([near[:, : 2 * HALO], near[:, rows:]], axis=1)
    qdocs = jnp.concatenate(
        [near[:, HALO + rows : HALO + rows + 1].T, jnp.full((EXTRA - 2, 1), -2.0, F32), near[:, HALO - 1 : HALO].T], axis=0
    )
    vm = pl.BlockSpec(memory_space=pltpu.VMEM)
    return pl.pallas_call(
        attention_kernel,
        out_shape=jax.ShapeDtypeStruct((rows + EXTRA, q.shape[1]), BF16),
        in_specs=[pl.BlockSpec(memory_space=pltpu.SMEM)] + [vm] * 8,
        out_specs=vm,
        scratch_shapes=[pltpu.VMEM((rows + 2 * HALO, q.shape[1]), BF16)],
        name="attend",
        cost_estimate=pl.CostEstimate(flops=8 * 10**8, bytes_accessed=10**6, transcendentals=10**6),
    )(sink_logits, q, qx, kv, kl, kr, docs, edocs, qdocs)


def project_kernel(tp_ref, *refs, blocks):
    att, weights = refs[:blocks], refs[blocks : 2 * blocks]
    res_ref, resx_ref, gain_ref, normed_ref, mine_ref, wide, stream, squares = refs[2 * blocks :]
    n = pl.program_id(0)
    steps = pl.num_programs(0)
    rows = res_ref.shape[0]
    cols = res_ref.shape[1]
    part = mine_ref.shape[0]

    @pl.when(n == 0)
    def _():
        for j, a in enumerate(att):
            wide[:, a.shape[1] * j : a.shape[1] * (j + 1)] = a[...]
        squares[...] = jnp.zeros_like(squares)

    w = jnp.concatenate([r[...] for r in weights], axis=0)
    proj = jnp.dot(wide[...], w, preferred_element_type=F32)
    at = pl.ds(pl.multiple_of(n * cols, cols), cols)
    for lo, hi, res in ((0, rows, res_ref), (rows, rows + EXTRA, resx_ref)):
        s = (res[...].astype(F32) + proj[lo:hi]).astype(BF16)
        stream[lo:hi, at] = s
        s = s.astype(F32)
        squares[lo:hi] += jnp.sum(s * s, axis=-1, keepdims=True)

    @pl.when(n == steps - 1)
    def _():
        full = stream.shape[1]
        scale = lax.rsqrt(squares[...] * (1.0 / full) + EPSILON)
        squares[...] = scale
        tile = 208
        for t in range(0, rows + EXTRA, tile):
            normed_ref[t : t + tile] = (
                stream[t : t + tile].astype(F32) * squares[t : t + tile] * gain_ref[...]
            ).astype(BF16)
        mine_ref[...] = stream[pl.ds(pl.multiple_of(tp_ref[0] * part, part), part), :]


def project(att, weights, residual, residual_x, gain, tp_index):
    rows, full = residual.shape
    all_rows = rows + EXTRA
    blocks = len(att)
    cols = 256
    part = rows // lax.axis_size("tp")
    k = sum(a.shape[1] for a in att)
    fixed = lambda shape: pl.BlockSpec(shape, lambda n, s: (0, 0))
    grid_spec = pltpu.PrefetchScalarGridSpec(
        num_scalar_prefetch=1,
        grid=(full // cols,),
        in_specs=[fixed(a.shape) for a in att]
        + [pl.BlockSpec((w.shape[0], cols), lambda n, s: (0, n)) for w in weights]
        + [
            pl.BlockSpec((rows, cols), lambda n, s: (0, n)),
            pl.BlockSpec((EXTRA, cols), lambda n, s: (0, n)),
            fixed((1, full)),
        ],
        out_specs=[fixed((all_rows, full)), fixed((part, full))],
        scratch_shapes=[
            pltpu.VMEM((all_rows, k), BF16),
            pltpu.VMEM((all_rows, full), BF16),
            pltpu.VMEM((all_rows, 1), F32),
        ],
    )
    return pl.pallas_call(
        functools.partial(project_kernel, blocks=blocks),
        grid_spec=grid_spec,
        out_shape=[
            jax.ShapeDtypeStruct((all_rows, full), BF16),
            jax.ShapeDtypeStruct((part, full), BF16),
        ],
        compiler_params=pltpu.CompilerParams(dimension_semantics=("arbitrary",), vmem_limit_bytes=BIG_VMEM),
        name="project",
        cost_estimate=pl.CostEstimate(flops=2 * all_rows * k * full, bytes_accessed=14 * 10**6, transcendentals=0),
    )(tp_index, *att, *weights, residual, residual_x, gain)


def copy_pieces(sources, places, offsets_ref, target, height, sem):
    copies = []
    for (ref, index), place in zip(sources, places):
        at = pl.ds(pl.multiple_of(offsets_ref[place] * height[0] + height[1], 16), height[2])
        c = pltpu.make_async_copy(ref.at[index], target.at[at, :], sem.at[len(copies)])
        c.start()
        copies.append(c)
    return copies


def gate_value_kernel(off_ref, normed_ref, same_ref, taps_ref, *refs, index_a, index_b):
    count = len(set(r for r, _, _ in index_a))
    a_refs, b_refs = refs[:count], refs[count : 2 * count]
    hidden_ref, gw, vw, gate, sems = refs[2 * count :]
    piece = gw.shape[0] // len(index_a)
    ga = copy_pieces([(a_refs[r], i) for r, i, _ in index_a], [p for _, _, p in index_a], off_ref, gw, (piece, 0, piece), sems.at[0])
    va = copy_pieces([(b_refs[r], i) for r, i, _ in index_b], [p for _, _, p in index_b], off_ref, vw, (piece, 0, piece), sems.at[1])
    rows = hidden_ref.shape[0]
    all_rows = normed_ref.shape[0]
    for c in ga:
        c.wait()
    tile = 208
    for t in range(0, all_rows, tile):
        g = jnp.dot(normed_ref[t : t + tile], gw[...], preferred_element_type=F32)
        gate[8 + t : 8 + t + tile] = g.astype(BF16).astype(F32)
    gate[7:8] = gate[8 + all_rows - 1 : 8 + all_rows]
    for c in va:
        c.wait()
    tile = 256
    for t in range(0, rows, tile):
        v = jnp.dot(normed_ref[t : t + tile], vw[...], preferred_element_type=F32)
        before = gate[7 + t : 7 + t + tile]
        here = gate[8 + t : 8 + t + tile]
        after = gate[9 + t : 9 + t + tile]
        conved = (
            taps_ref[0:1] * before * same_ref[t : t + tile, 0:1]
            + taps_ref[1:2] * here
            + taps_ref[2:3] * after * same_ref[t : t + tile, 1:2]
        )
        hidden_ref[t : t + tile] = (jax.nn.gelu(conved, approximate=True) * v).astype(BF16)


def gate_value(normed, same, taps, a, b, index_a, index_b, offsets, rows):
    full = normed.shape[1]
    units = taps.shape[1]
    vm = pl.BlockSpec(memory_space=pltpu.VMEM)
    hbm = pl.BlockSpec(memory_space=pl.ANY)
    return pl.pallas_call(
        functools.partial(gate_value_kernel, index_a=index_a, index_b=index_b),
        out_shape=jax.ShapeDtypeStruct((rows, units), BF16),
        in_specs=[pl.BlockSpec(memory_space=pltpu.SMEM), vm, vm, vm] + [hbm] * (len(a) + len(b)),
        out_specs=vm,
        scratch_shapes=[
            pltpu.VMEM((full, units), BF16),
            pltpu.VMEM((full, units), BF16),
            pltpu.VMEM((normed.shape[0] + 16, units), F32),
            pltpu.SemaphoreType.DMA((2, len(index_a))),
        ],
        compiler_params=pltpu.CompilerParams(vmem_limit_bytes=BIG_VMEM),
        name="gate_value",
        cost_estimate=pl.CostEstimate(flops=4 * rows * full * units, bytes_accessed=12 * 10**6, transcendentals=10**6),
    )(offsets, normed, same, taps, *a, *b)


def down_kernel(off_ref, core_ref, hidden_ref, *refs, index_a, index_b):
    count = len(set(r for r, _, _ in index_a))
    a_refs, b_refs = refs[:count], refs[count : 2 * count]
    send_ref, keep_ref, dw, picked, sems = refs[2 * count :]
    piece = dw.shape[0] // len(index_a)
    half = piece // 2
    copies = copy_pieces([(a_refs[r], i) for r, i, _ in index_a], [p for _, _, p in index_a], off_ref, dw, (piece, 0, half), sems.at[0])
    copies += copy_pieces([(b_refs[r], i) for r, i, _ in index_b], [p for _, _, p in index_b], off_ref, dw, (piece, half, half), sems.at[1])
    part = send_ref.shape[1]
    nx = send_ref.shape[0]
    core = core_ref[0]
    for k in range(nx):
        for which, slot in ((1 - core, 0), (core, 1)):
            at = pl.ds(pl.multiple_of((2 * k + which) * part, part), part)
            picked[slot, part * k : part * (k + 1), :] = hidden_ref[at, :]
    for c in copies:
        c.wait()
    cols = 512
    for slot, out in ((0, send_ref), (1, keep_ref)):
        for n in range(0, dw.shape[0], cols):
            r = lax.dot_general(picked[slot], dw[n : n + cols, :], LAST, preferred_element_type=F32)
            for k in range(nx):
                out[k, :, n : n + cols] = r[part * k : part * (k + 1)].astype(BF16)


def down(hidden, a, b, index_a, index_b, offsets, core, nx, full):
    rows, units = hidden.shape
    part = rows // (2 * nx)
    vm = pl.BlockSpec(memory_space=pltpu.VMEM)
    hbm = pl.BlockSpec(memory_space=pl.ANY)
    sm = pl.BlockSpec(memory_space=pltpu.SMEM)
    shape = jax.ShapeDtypeStruct((nx, part, full), BF16)
    return pl.pallas_call(
        functools.partial(down_kernel, index_a=index_a, index_b=index_b),
        out_shape=[shape, shape],
        in_specs=[sm, sm, vm] + [hbm] * (len(a) + len(b)),
        out_specs=[vm, vm],
        scratch_shapes=[
            pltpu.VMEM((full, units), BF16),
            pltpu.VMEM((2, rows // 2, units), BF16),
            pltpu.SemaphoreType.DMA((2, len(index_a))),
        ],
        compiler_params=pltpu.CompilerParams(vmem_limit_bytes=BIG_VMEM),
        name="down",
        cost_estimate=pl.CostEstimate(flops=2 * rows * full * units, bytes_accessed=8 * 10**6, transcendentals=0),
    )(offsets, core, hidden, *a, *b)


def pair_sum_kernel(x_ref, keep_ref, got_ref, *outs):
    nx = keep_ref.shape[0]
    x = x_ref[0]
    for d, out in enumerate(outs):
        k = lax.rem(x + d, nx)
        out[...] = (keep_ref[k].astype(F32) + got_ref[k].astype(F32)).astype(BF16)


def pair_sum(keep, got, x):
    nx, part, full = keep.shape
    vm = pl.BlockSpec(memory_space=pltpu.VMEM)
    shape = jax.ShapeDtypeStruct((part, full), BF16)
    return pl.pallas_call(
        pair_sum_kernel,
        out_shape=[shape] * nx,
        in_specs=[pl.BlockSpec(memory_space=pltpu.SMEM), vm, vm],
        out_specs=[vm] * nx,
        compiler_params=pltpu.CompilerParams(vmem_limit_bytes=BIG_VMEM),
        name="pair_sum",
    )(x, keep, got)


def first_phase(x, shift):
    back = shift(x, 1)
    ahead = shift(x, -1)
    far = shift(x, 2)
    return jnp.stack([x, back, ahead, far])


def second_phase(block, shift):
    back = shift(block, 1)
    ahead = shift(block, -1)
    far_low = shift(back[:2], 1)
    far_high = shift(ahead[2:], -1)
    return [block, back, ahead, far_low, far_high]


STEPS = (0, -1, 1, 2)


def piece_index(first_is_z):
    index = []
    for array, steps in enumerate((0, 1, 2)):
        for i in range(4):
            index.append((array, i, (i * 4 + steps) if first_is_z else (steps * 4 + i)))
    for array, lo in ((3, 0), (4, 2)):
        for i in range(2):
            f = lo + i
            index.append((array, i, (f * 4 + 3) if first_is_z else (3 * 4 + f)))
    return tuple(index)


def on_device(
    queries,
    keys_values,
    sink_logits,
    doc_ids,
    residual,
    out_weight,
    ffn_gain,
    gate_weight,
    value_weight,
    conv_taps,
    down_weight,
    *,
    nz,
    ny,
):
    rows, full = residual.shape
    nx = lax.axis_size("tp") // 2
    sp_count = nz * ny
    sp = lax.axis_index("sp")
    tp = lax.axis_index("tp")
    offset = sp * rows
    q = queries.reshape(rows, -1)
    kv = keys_values.reshape(rows, -1)

    def halo(lo_kv, q_row, res_row):
        return jnp.concatenate([lo_kv, q_row, jnp.zeros((15, q.shape[1]), BF16), res_row.reshape(-1, q.shape[1])], axis=0)

    ring_up = [(i, (i + 1) % sp_count) for i in range(sp_count)]
    ring_down = [((i + 1) % sp_count, i) for i in range(sp_count)]
    left = lax.ppermute(halo(kv[rows - HALO :], q[rows - 1 :], residual[rows - 1 :]), "sp", ring_up)
    right = lax.ppermute(halo(kv[:HALO], q[:1], residual[:1]), "sp", ring_down)

    half = down_weight.shape[0] // 2
    piece = gate_weight.shape[0]
    along_z = lambda x, d: grid_shift(x, d, 0, nz, ny)
    along_y = lambda x, d: grid_shift(x, 0, d, nz, ny)
    a = first_phase(jnp.concatenate([gate_weight, down_weight[:half]], axis=0), along_z)
    b = first_phase(jnp.concatenate([value_weight, down_weight[half:]], axis=0), along_y)
    gates = second_phase(a[:, :piece], along_y)
    values = second_phase(b[:, :piece], along_z)
    downs_a = second_phase(a[:, piece:], along_y)
    downs_b = second_phase(b[:, piece:], along_z)
    index_a, index_b = piece_index(True), piece_index(False)
    z, y = sp // ny, sp % ny
    steps = jnp.array(STEPS, jnp.int32)
    offsets = (((z + steps) % nz)[:, None] * ny + ((y + steps) % ny)[None, :]).reshape(-1).astype(jnp.int32)

    o = [out_weight] + [tp_shift(out_weight, d, False, nx) for d in (1, -1, 2)]
    o = o + [swap_cores(w) for w in o]

    docs_f = jnp.pad(doc_ids.astype(F32), HALO, constant_values=-1.0)
    att = attend(q, kv, sink_logits, docs_f, offset, left, right)
    t = [att] + [tp_shift(att, d, False, nx) for d in (1, -1, 2)]
    t = t + [swap_cores(w) for w in t]

    res_rows = lambda h: h[HALO + 16 :].reshape(1, full)
    residual_x = jnp.concatenate([res_rows(right), jnp.zeros((EXTRA - 2, full), BF16), res_rows(left)], axis=0)
    normed, mine = project(t, o, residual, residual_x, ffn_gain[None], tp.reshape(1))

    near = lax.dynamic_slice_in_dim(docs_f, offset + HALO - 1, rows + 2)
    same = jnp.stack([near[1:-1] == near[:-2], near[1:-1] == near[2:]], axis=1).astype(F32)
    hidden = gate_value(normed, same, conv_taps, gates, values, index_a, index_b, offsets, rows)
    send, keep = down(hidden, downs_a, downs_b, index_a, index_b, offsets, (tp % 2).reshape(1), nx, full)
    got = swap_cores(send)
    own, ahead, far, back = pair_sum(keep, got, (tp // 2).reshape(1))
    parts = [own, tp_shift(ahead, 1, False, nx), tp_shift(back, -1, False, nx), tp_shift(far, 2, False, nx)]
    total = mine.astype(F32)
    for p in parts:
        total = total + p.astype(F32)
    return total.astype(BF16)


def solution(mesh):
    in_specs = (
        P("sp", "tp", None),
        P("sp", "tp", None),
        P("tp", None),
        P(),
        P("sp", None),
        P("tp", None),
        P(),
        P("sp", "tp"),
        P("sp", "tp"),
        P(None, "tp"),
        P("sp", "tp"),
    )
    out_specs = P(("sp", "tp"), None)
    return jax.shard_map(
        functools.partial(on_device, nz=4, ny=4), mesh=mesh, in_specs=in_specs, out_specs=out_specs, check_vma=False
    )
```

```python
import functools

import jax
import jax.numpy as jnp
from jax import lax
from jax.experimental import pallas as pl
from jax.experimental.pallas import tpu as pltpu
from jax.sharding import PartitionSpec as P


WINDOW = 128
HEAD_DIM = 64
HALO = 144
EXTRA = 16
EPSILON = 1e-06
MASKED = -1e30
F32 = jnp.float32
BF16 = jnp.bfloat16
MIB = 1024 * 1024
LAST = (((1,), (1,)), ((), ()))


VM = pl.BlockSpec(memory_space=pltpu.VMEM)
ANY = pl.BlockSpec(memory_space=pl.ANY)
SM = pl.BlockSpec(memory_space=pltpu.SMEM)


def call(kernel, name, out, args, specs, vmem, scratch=(), flops=0):
    shapes = [jax.ShapeDtypeStruct(s, d) for s, d in out]
    return pl.pallas_call(
        kernel,
        out_shape=shapes,
        in_specs=specs,
        out_specs=[VM] * len(shapes),
        scratch_shapes=list(scratch),
        compiler_params=pltpu.CompilerParams(vmem_limit_bytes=vmem * MIB),
        name=name,
        cost_estimate=pl.CostEstimate(flops=flops, bytes_accessed=10**6, transcendentals=0),
    )(*args)


def grid_shift(x, dz, dy, nz, ny):
    perm = [(z * ny + y, ((z + dz) % nz) * ny + (y + dy) % ny) for z in range(nz) for y in range(ny)]
    return lax.ppermute(x, "sp", perm)


def core_shift(x, along_z, nz, ny, ntp):
    perm = []
    for z in range(nz):
        for y in range(ny):
            for t in range(ntp):
                d = 1 if t % 2 == 0 else -1
                to = ((z + d) % nz) * ny + y if along_z else z * ny + (y + d) % ny
                perm.append(((z * ny + y) * ntp + t, to * ntp + t))
    return lax.ppermute(x, ("sp", "tp"), perm)


def tp_shift(x, dx, swap, nx):
    perm = [
        (i * 2 + c, ((i + dx) % nx) * 2 + (1 - c if swap else c)) for i in range(nx) for c in range(2)
    ]
    return lax.ppermute(x, "tp", perm)


def swap_cores(x):
    return tp_shift(x, 0, True, lax.axis_size("tp") // 2)


def prepare_kernel(q_ref, kv_ref, first_ref, last_ref, gate_ref, value_ref, down_ref, up_ref, dn_ref, a_ref, b_ref):
    rows = kv_ref.shape[0]
    lanes = kv_ref.shape[1]
    edge = first_ref.shape[0]
    for out, kv_at, row, res, res_row in (
        (up_ref, rows - HALO, rows - 1, last_ref, edge - 1),
        (dn_ref, 0, 0, first_ref, 0),
    ):
        out[0:HALO] = kv_ref[kv_at : kv_at + HALO]
        near = 0 if row == 0 else rows - EXTRA
        out[HALO : HALO + EXTRA] = q_ref[near : near + EXTRA]
        tile = jnp.concatenate(
            [res[res_row : res_row + 1, lanes * j : lanes * (j + 1)] for j in range(res.shape[1] // lanes)], axis=0
        )
        out[HALO + EXTRA :] = tile
    piece = gate_ref.shape[0]
    half = down_ref.shape[0] // 2
    for out, w, lo in ((a_ref, gate_ref, 0), (b_ref, value_ref, half)):
        out[0:piece] = w[...]
        out[piece:] = down_ref[lo : lo + half]


def prepare(q, kv, residual, gate, value, down_w):
    rows, lanes = kv.shape
    full = residual.shape[1]
    whole = lambda a: pl.BlockSpec(a.shape, lambda i: (0, 0))
    out = [(HALO + EXTRA + full // lanes, lanes)] * 2 + [(gate.shape[0] + down_w.shape[0] // 2, gate.shape[1])] * 2
    return pl.pallas_call(
        prepare_kernel,
        grid=(1,),
        out_shape=[jax.ShapeDtypeStruct(s, BF16) for s in out],
        in_specs=[
            whole(q),
            whole(kv),
            pl.BlockSpec((EXTRA, full), lambda i: (0, 0)),
            pl.BlockSpec((EXTRA, full), lambda i: (rows // EXTRA - 1, 0)),
            whole(gate),
            whole(value),
            whole(down_w),
        ],
        out_specs=[pl.BlockSpec(s, lambda i: (0, 0)) for s in out],
        compiler_params=pltpu.CompilerParams(vmem_limit_bytes=8 * MIB),
        name="prepare",
    )(q, kv, residual, residual, gate, value, down_w)


def pack_kernel(*refs):
    ins, (g_ref, d_ref) = refs[:-2], refs[-2:]
    piece = g_ref.shape[2]
    n = len(ins) // 2
    for c in range(2):
        for i in range(n):
            g_ref[c, i] = ins[c * n + i][0:piece]
            d_ref[c, i] = ins[c * n + i][piece:]


def pack(own, other, piece):
    n = len(own)
    rows, units = own[0].shape
    return call(
        pack_kernel,
        "pack",
        [((2, n, piece, units), BF16), ((2, n, rows - piece, units), BF16)],
        (*own, *other),
        [VM] * (2 * n),
        6,
    )


def document_row(docs_ref, index):
    count = docs_ref.shape[0]
    inside = ((index >= 0) & (index < count)).astype(jnp.int32)
    row = docs_ref[pl.ds(jnp.clip(index, 0, count - 1), 1), :]
    return (row * inside + (inside - 1)).astype(F32)


def column(row, n):
    return jnp.transpose(jnp.broadcast_to(row, (n, row.shape[1])))


def attention_kernel(at_ref, sink_ref, q_ref, kv_ref, kl_ref, kr_ref, docs_ref, out_ref, kvx):
    rows = q_ref.shape[0]
    w = WINDOW
    width = 2 * HEAD_DIM
    blocks = rows // w
    kvx[0:HALO] = kl_ref[0:HALO]
    kvx[HALO : HALO + rows] = kv_ref[...]
    kvx[HALO + rows :] = kr_ref[0:HALO]
    base = at_ref[0] * blocks
    docs = {k: document_row(docs_ref, base + k) for k in range(-2, blocks + 2)}

    def heads(items):
        parts = []
        for q, keys, allowed in items:
            low = lax.broadcasted_iota(jnp.int32, q.shape, 1) < HEAD_DIM
            swapped = jnp.concatenate([q[:, HEAD_DIM:], q[:, :HEAD_DIM]], axis=1)
            zero = jnp.zeros_like(q)
            parts.append((jnp.where(low, q, zero), keys, allowed, sink_ref[0, 0]))
            parts.append((jnp.where(low, swapped, zero), keys, allowed, sink_ref[0, 1]))
        scores = [
            lax.dot_general(q, keys, LAST, preferred_element_type=F32) * HEAD_DIM**-0.5 for q, keys, _, _ in parts
        ]
        scores = [jnp.where(p[2], s, MASKED) for s, p in zip(scores, parts)]
        tops = [jnp.maximum(jnp.max(s, axis=-1, keepdims=True), p[3]) for s, p in zip(scores, parts)]
        exps = [jnp.exp(s - t) for s, t in zip(scores, tops)]
        totals = [jnp.sum(e, axis=-1, keepdims=True) + jnp.exp(p[3] - t) for e, t, p in zip(exps, tops, parts)]
        outs = [
            jnp.dot(e.astype(BF16), p[1], preferred_element_type=F32) * (1.0 / t)
            for e, t, p in zip(exps, totals, parts)
        ]
        results = []
        for j in range(len(items)):
            a, b = outs[2 * j], outs[2 * j + 1]
            low = lax.broadcasted_iota(jnp.int32, a.shape, 1) < HEAD_DIM
            first = jnp.concatenate([a[:, HEAD_DIM:], a[:, :HEAD_DIM]], axis=1)
            results.append(jnp.where(low, first, b).astype(BF16))
        return results

    away = lax.broadcasted_iota(jnp.int32, (w, 3 * w), 0) + w - lax.broadcasted_iota(jnp.int32, (w, 3 * w), 1)
    near = jnp.abs(away) <= WINDOW
    group = 4
    for first in range(0, blocks, group):
        items = []
        for i in range(first, first + group):
            own = jnp.concatenate([column(docs[i], w)] * 3, axis=1)
            allowed = near & (own == jnp.concatenate([docs[i - 1], docs[i], docs[i + 1]], axis=1))
            start = HALO - w + w * i
            items.append((q_ref[w * i : w * (i + 1)], kvx[start : start + 3 * w], allowed))
        for i, r in zip(range(first, first + group), heads(items)):
            out_ref[w * i : w * (i + 1)] = r

    span = 2 * HALO
    lead = 2 * w - HALO
    keys = jnp.concatenate([kvx[0:span], kvx[rows : rows + span]], axis=0)
    key_docs = jnp.concatenate(
        [
            jnp.concatenate([docs[k + j] for j in range(4)], axis=1)[:, lead : lead + span]
            for k in (-2, blocks - 2)
        ],
        axis=1,
    )
    row = lax.broadcasted_iota(jnp.int32, (EXTRA, 2 * span), 0)
    col = lax.broadcasted_iota(jnp.int32, (EXTRA, 2 * span), 1)
    key_at = jnp.where(col < span, col - HALO, col - span + rows - HALO)
    at = jnp.where(row == 0, rows, -1)
    own = jnp.where(row == 0, docs[blocks][:, 0:1], docs[-1][:, w - 1 : w])
    allowed = (jnp.abs(at - key_at) <= WINDOW) & (own == key_docs)
    qrow = lax.broadcasted_iota(jnp.int32, (EXTRA, width), 0)
    ahead = kr_ref[HALO : HALO + EXTRA].astype(F32)
    behind = kl_ref[HALO : HALO + EXTRA].astype(F32)
    qx = jnp.where(qrow == 0, ahead, behind).astype(BF16)
    out_ref[rows : rows + EXTRA] = heads([(qx, keys, allowed)])[0]


def attend(q, kv, sink_logits, doc_table, sp, left, right):
    rows, width = q.shape
    return call(
        attention_kernel,
        "attend",
        [((rows + EXTRA, width), BF16)],
        (sp, sink_logits, q, kv, left, right, doc_table),
        [SM, SM] + [VM] * 5,
        8,
        [pltpu.VMEM((rows + 2 * HALO, width), BF16)],
        flops=10**9,
    )[0]


def same_kernel(at_ref, docs_ref, out_ref):
    w = docs_ref.shape[1]
    blocks = out_ref.shape[0] // w
    base = at_ref[0] * blocks
    lane = lax.broadcasted_iota(jnp.int32, (1, w), 1)
    docs = {k: document_row(docs_ref, base + k) for k in range(-1, blocks + 1)}
    for i in range(blocks):
        before = jnp.where(lane == 0, pltpu.roll(docs[i - 1], 1, 1), pltpu.roll(docs[i], 1, 1))
        after = jnp.where(lane == w - 1, pltpu.roll(docs[i + 1], w - 1, 1), pltpu.roll(docs[i], w - 1, 1))
        out_ref[w * i : w * (i + 1), 0:w] = column((before == docs[i]).astype(F32), w)
        out_ref[w * i : w * (i + 1), w : 2 * w] = column((after == docs[i]).astype(F32), w)


def project_kernel(tp_ref, *refs, blocks):
    att, weights = refs[:blocks], refs[blocks : 2 * blocks]
    res_ref, left_ref, right_ref, gain_ref, normed_ref, mine_ref, wide, deep, stream, squares = refs[2 * blocks :]
    rows, full = res_ref.shape
    lanes = left_ref.shape[1]
    part = mine_ref.shape[0]
    cols = 256
    for j in range(blocks):
        wide[:, lanes * j : lanes * (j + 1)] = att[j][...]
        deep[lanes * j : lanes * (j + 1)] = weights[j][...]
    squares[...] = jnp.zeros_like(squares)
    top = HALO + EXTRA
    row = lax.broadcasted_iota(jnp.int32, (EXTRA, cols), 0)
    for n in range(full // cols):
        proj = jnp.dot(wide[...], deep[:, cols * n : cols * (n + 1)], preferred_element_type=F32)
        j = top + n * (cols // lanes)
        ahead = jnp.concatenate([right_ref[j + i : j + i + 1] for i in range(cols // lanes)], axis=1).astype(F32)
        behind = jnp.concatenate([left_ref[j + i : j + i + 1] for i in range(cols // lanes)], axis=1).astype(F32)
        outer = jnp.where(row == 0, ahead, behind)
        for lo, hi, res in (
            (0, rows, res_ref[:, cols * n : cols * (n + 1)].astype(F32)),
            (rows, rows + EXTRA, outer),
        ):
            s = (res + proj[lo:hi]).astype(BF16)
            stream[lo:hi, cols * n : cols * (n + 1)] = s
            s = s.astype(F32)
            s = s * s
            squares[lo:hi] += s[:, :lanes] + s[:, lanes:]
    scale = lax.rsqrt(jnp.sum(squares[...], axis=-1, keepdims=True) * (1.0 / full) + EPSILON)
    squares[...] = jnp.broadcast_to(scale, squares.shape)
    tile = 208
    for t in range(0, rows + EXTRA, tile):
        for n in range(full // lanes):
            c = slice(lanes * n, lanes * (n + 1))
            normed_ref[t : t + tile, c] = (
                stream[t : t + tile, c].astype(F32) * squares[t : t + tile] * gain_ref[:, c]
            ).astype(BF16)
    mine_ref[...] = stream[pl.ds(pl.multiple_of(tp_ref[0] * part, part), part), :]


def project(att, weights, residual, left, right, gain, tp_index):
    rows, full = residual.shape
    all_rows = rows + EXTRA
    blocks = len(att)
    lanes = att[0].shape[1]
    part = rows // lax.axis_size("tp")
    k = lanes * blocks
    return call(
        functools.partial(project_kernel, blocks=blocks),
        "project",
        [((all_rows, full), BF16), ((part, full), BF16)],
        (tp_index, *att, *weights, residual, left, right, gain),
        [SM] + [VM] * (2 * blocks + 4),
        20,
        [
            pltpu.VMEM((all_rows, k), BF16),
            pltpu.VMEM((k, full), BF16),
            pltpu.VMEM((all_rows, full), BF16),
            pltpu.VMEM((all_rows, lanes), F32),
        ],
        flops=2 * all_rows * k * full,
    )


def copy_pieces(sources, offsets_ref, target, stride, shift, height, sem):
    copies = []
    for j, (ref, index, place) in enumerate(sources):
        at = pl.ds(pl.multiple_of(offsets_ref[place] * stride + shift, 16), height)
        c = pltpu.make_async_copy(ref.at[index], target.at[at, :], sem.at[j])
        c.start()
        copies.append(c)
    return copies


def sources_of(refs):
    n = refs[0].shape[1]
    found = []
    for slot, ref in enumerate(refs):
        for i in range(n):
            found.append((ref, (0, i) if slot < 2 else (i,), i * 4 + slot))
    return found


def gate_value_kernel(off_ref, normed_ref, same_ref, taps_ref, *refs):
    a_refs, b_refs = refs[:4], refs[4:8]
    hidden_ref, gw, vw, both, sems = refs[8:]
    a, b = sources_of(a_refs), sources_of(b_refs)
    piece = gw.shape[0] // len(a)
    copies = copy_pieces(a, off_ref.at[0], gw, piece, 0, piece, sems.at[0])
    copies += copy_pieces(b, off_ref.at[1], vw, piece, 0, piece, sems.at[1])
    rows, units = hidden_ref.shape
    all_rows = normed_ref.shape[0]
    lanes = 128
    for c in copies:
        c.wait()
    tile = 256
    for n in range(units // lanes):
        cs = slice(lanes * n, lanes * (n + 1))
        slot = n % 2
        w = jnp.concatenate([gw[:, cs], vw[:, cs]], axis=1)
        r = jnp.dot(normed_ref[...], w, preferred_element_type=F32)
        both[slot, 8 : 8 + all_rows, :lanes] = r[:, :lanes].astype(BF16).astype(F32)
        both[slot, 8 : 8 + all_rows, lanes:] = r[:, lanes:]
        both[slot, 7:8, :lanes] = both[slot, 7 + all_rows : 8 + all_rows, :lanes]
        for t in range(0, rows, tile):
            conved = (
                taps_ref[0:1, cs] * both[slot, 7 + t : 7 + t + tile, :lanes] * same_ref[t : t + tile, :lanes]
                + taps_ref[1:2, cs] * both[slot, 8 + t : 8 + t + tile, :lanes]
                + taps_ref[2:3, cs] * both[slot, 9 + t : 9 + t + tile, :lanes] * same_ref[t : t + tile, lanes:]
            )
            value = both[slot, 8 + t : 8 + t + tile, lanes:]
            hidden_ref[t : t + tile, cs] = (jax.nn.gelu(conved, approximate=True) * value).astype(BF16)


def gate_value(normed, same, taps, a, b, offsets, rows):
    all_rows, full = normed.shape
    units = taps.shape[1]
    pieces = 4 * a[0].shape[1]
    return call(
        gate_value_kernel,
        "gate_value",
        [((rows, units), BF16)],
        (offsets, normed, same, taps, *a, *b),
        [SM, VM, VM, VM] + [ANY] * 8,
        16,
        [
            pltpu.VMEM((full, units), BF16),
            pltpu.VMEM((full, units), BF16),
            pltpu.VMEM((2, all_rows + 16, 256), F32),
            pltpu.SemaphoreType.DMA((2, pieces)),
        ],
        flops=4 * rows * full * units,
    )[0]


def down_send_kernel(off_ref, core_ref, hidden_ref, *refs):
    a_refs, b_refs = refs[:4], refs[4:8]
    outs, dw_ref, keep_ref, picked, sems = refs[8:-4], refs[-4], refs[-3], refs[-2], refs[-1]
    a, b = sources_of(a_refs), sources_of(b_refs)
    piece = dw_ref.shape[0] // len(a)
    half = piece // 2
    copies = copy_pieces(a, off_ref.at[0], dw_ref, piece, 0, half, sems.at[0])
    copies += copy_pieces(b, off_ref.at[1], dw_ref, piece, half, half, sems.at[1])
    nx, part, cols = outs[0].shape
    core = core_ref[0]
    for k in range(nx):
        for which, target in ((1 - core, picked), (core, keep_ref)):
            at = pl.ds(pl.multiple_of((2 * k + which) * part, part), part)
            target[part * k : part * (k + 1), :] = hidden_ref[at, :]
    for c in copies:
        c.wait()
    wide = 256
    for h, out in enumerate(outs):
        for n in range(0, cols, wide):
            at = h * cols + n
            r = lax.dot_general(picked[...], dw_ref[at : at + wide, :], LAST, preferred_element_type=F32)
            for k in range(nx):
                out[k, :, n : n + wide] = r[part * k : part * (k + 1)].astype(BF16)


def down_send(hidden, a, b, offsets, core, nx, full, chunks):
    rows, units = hidden.shape
    part = rows // (2 * nx)
    pieces = 4 * a[0].shape[1]
    out = call(
        down_send_kernel,
        "down_send",
        [((nx, part, full // chunks), BF16)] * chunks + [((full, units), BF16), ((rows // 2, units), BF16)],
        (offsets, core, hidden, *a, *b),
        [SM, SM, VM] + [ANY] * 8,
        8,
        [pltpu.VMEM((rows // 2, units), BF16), pltpu.SemaphoreType.DMA((2, pieces))],
        flops=rows * full * units,
    )
    return out[:chunks], out[chunks], out[chunks + 1]


def down_keep_kernel(x_ref, keep_ref, dw_ref, got_ref, *refs, first):
    outs, acc = refs[:-1], refs[-1]
    nx, part, cols = got_ref.shape
    wide = 256
    for n in range(0, cols, wide):
        at = first + n
        r = lax.dot_general(keep_ref[...], dw_ref[at : at + wide, :], LAST, preferred_element_type=F32)
        for k in range(nx):
            acc[k, :, n : n + wide] = (r[part * k : part * (k + 1)] + got_ref[k, :, n : n + wide].astype(F32)).astype(BF16)
    for d, out in enumerate(outs):
        out[...] = acc[lax.rem(x_ref[0] + d, nx)]


def down_keep(keep, dw, got, x, first):
    nx, part, cols = got.shape
    return call(
        functools.partial(down_keep_kernel, first=first),
        "down_keep",
        [((part, cols), BF16)] * nx,
        (x, keep, dw, got),
        [SM, VM, VM, VM],
        6,
        [pltpu.VMEM((nx, part, cols), BF16)],
        flops=2 * keep.shape[0] * keep.shape[1] * cols,
    )


def total_kernel(mine_ref, *refs):
    ins, out_ref = refs[:-1], refs[-1]
    chunks = len(ins) // 4
    cols = ins[0].shape[1]
    for h in range(chunks):
        s = mine_ref[:, cols * h : cols * (h + 1)].astype(F32)
        for r in ins[4 * h : 4 * h + 4]:
            s = s + r[...].astype(F32)
        out_ref[:, cols * h : cols * (h + 1)] = s.astype(BF16)


CHUNKS = 2


def on_device(
    queries,
    keys_values,
    sink_logits,
    doc_ids,
    residual,
    out_weight,
    ffn_gain,
    gate_weight,
    value_weight,
    conv_taps,
    down_weight,
    *,
    nz,
    ny,
):
    rows, full = residual.shape
    ntp = lax.axis_size("tp")
    nx = ntp // 2
    sp_count = nz * ny
    sp = lax.axis_index("sp")
    tp = lax.axis_index("tp")
    core = tp % 2
    q = queries.reshape(rows, -1)
    kv = keys_values.reshape(rows, -1)
    doc_table = doc_ids.reshape(-1, 128)
    one = lambda v: v.reshape(1).astype(jnp.int32)
    piece = gate_weight.shape[0]

    halo_up, halo_down, stack_a, stack_b = prepare(q, kv, residual, gate_weight, value_weight, down_weight)

    o = [out_weight] + [tp_shift(out_weight, d, False, nx) for d in (1, -1, 2)]
    o = o + [swap_cores(w) for w in o]

    ring_up = [(i, (i + 1) % sp_count) for i in range(sp_count)]
    ring_down = [((i + 1) % sp_count, i) for i in range(sp_count)]
    left = lax.ppermute(halo_up, "sp", ring_up)
    right = lax.ppermute(halo_down, "sp", ring_down)

    def ring(stack, along_z):
        shift = (lambda x, d: grid_shift(x, d, 0, nz, ny)) if along_z else (lambda x, d: grid_shift(x, 0, d, nz, ny))
        return [stack] + [shift(stack, d) for d in (1, -1, 2)]

    def plane(block, along_z):
        got = core_shift(block, along_z, nz, ny, ntp)
        return [block, got, swap_cores(got[1]), core_shift(got[0], along_z, nz, ny, ntp)]

    ring_a, ring_b = ring(stack_a, True), ring(stack_b, False)
    gate_block, down_block_a = pack(ring_a, [swap_cores(p) for p in ring_a], piece)
    value_block, down_block_b = pack(ring_b, [swap_cores(p) for p in ring_b], piece)
    gates, values = plane(gate_block, False), plane(value_block, True)
    downs_a, downs_b = plane(down_block_a, False), plane(down_block_b, True)
    z, y = sp // ny, sp % ny
    first = jnp.array((0, -1, 1, 2), jnp.int32)
    up = jnp.where(core == 0, -1, 1)
    second = jnp.stack([0 * up, up, -up, 0 * up + 2]).astype(jnp.int32)
    place = lambda dz, dy: (((z + dz) % nz) * ny + (y + dy) % ny).reshape(-1)
    offsets = jnp.stack([place(first[:, None], second[None]), place(second[None], first[:, None])]).astype(jnp.int32)

    att = attend(q, kv, sink_logits, doc_table, one(sp), left, right)
    t = [att] + [tp_shift(att, d, False, nx) for d in (1, -1, 2)]
    t = t + [swap_cores(w) for w in t]
    same = call(same_kernel, "same", [((rows, 256), F32)], (one(sp), doc_table), [SM, VM], 4)[0]

    normed, mine = project(t, o, residual, left, right, ffn_gain[None], one(tp))
    hidden = gate_value(normed, same, conv_taps, gates, values, offsets, rows)
    sends, dw, keep = down_send(hidden, downs_a, downs_b, offsets, one(core), nx, full, CHUNKS)
    gots = [swap_cores(s) for s in sends]
    parts = []
    for h, got in enumerate(gots):
        own, ahead, far, back = down_keep(keep, dw, got, one(tp // 2), h * (full // CHUNKS))
        parts += [own, tp_shift(ahead, 1, False, nx), tp_shift(back, -1, False, nx), tp_shift(far, 2, False, nx)]
    return call(total_kernel, "total", [(mine.shape, BF16)], (mine, *parts), [VM] * (1 + len(parts)), 4)[0]


def solution(mesh):
    in_specs = (
        P("sp", "tp", None),
        P("sp", "tp", None),
        P("tp", None),
        P(),
        P("sp", None),
        P("tp", None),
        P(),
        P("sp", "tp"),
        P("sp", "tp"),
        P(None, "tp"),
        P("sp", "tp"),
    )
    out_specs = P(("sp", "tp"), None)
    return jax.shard_map(
        functools.partial(on_device, nz=4, ny=4), mesh=mesh, in_specs=in_specs, out_specs=out_specs, check_vma=False
    )
```

```python
import functools

import jax
import jax.numpy as jnp
from jax import lax
from jax.experimental import pallas as pl
from jax.experimental.pallas import tpu as pltpu
from jax.sharding import PartitionSpec as P


WINDOW = 128
HEAD_DIM = 64
HALO = 144
EXTRA = 16
EPSILON = 1e-06
MASKED = -1e30
F32 = jnp.float32
BF16 = jnp.bfloat16
MIB = 1024 * 1024
LAST = (((1,), (1,)), ((), ()))


NZ, NY = 4, 4
VM = pl.BlockSpec(memory_space=pltpu.VMEM)
ANY = pl.BlockSpec(memory_space=pl.ANY)
SM = pl.BlockSpec(memory_space=pltpu.SMEM)


def call(kernel, out, args, specs, vmem, scratch=(), flops=0):
    shapes = [jax.ShapeDtypeStruct(s, d) for s, d in out]
    return pl.pallas_call(
        kernel,
        out_shape=shapes,
        in_specs=specs,
        out_specs=[VM] * len(shapes),
        scratch_shapes=list(scratch),
        compiler_params=pltpu.CompilerParams(vmem_limit_bytes=vmem * MIB),
        cost_estimate=pl.CostEstimate(flops=flops, bytes_accessed=10**6, transcendentals=0),
    )(*args)


def grid_shift(x, dz, dy, nz, ny):
    perm = [(z * ny + y, ((z + dz) % nz) * ny + (y + dy) % ny) for z in range(nz) for y in range(ny)]
    return lax.ppermute(x, "sp", perm)


def core_shift(x, axis, nz, ny, nx):
    perm = []
    at = lambda z, y, i, c: ((z % nz) * ny + y % ny) * 2 * nx + (i % nx) * 2 + c
    for z in range(nz):
        for y in range(ny):
            for i in range(nx):
                for c in range(2):
                    d = 1 - 2 * c
                    to = {"z": (z + d, y, i, c), "y": (z, y + d, i, c), "x": (z, y, i + d, c)}[axis]
                    perm.append((at(z, y, i, c), at(*to)))
    return lax.ppermute(x, ("sp", "tp"), perm)


def tp_shift(x, dx, swap, nx):
    perm = [
        (i * 2 + c, ((i + dx) % nx) * 2 + (1 - c if swap else c)) for i in range(nx) for c in range(2)
    ]
    return lax.ppermute(x, "tp", perm)


def swap_cores(x):
    return tp_shift(x, 0, True, lax.axis_size("tp") // 2)


def prepare_kernel(q_ref, kv_ref, res_ref, gate_ref, value_ref, down_ref, up_ref, dn_ref, a_ref, b_ref, edges, sems):
    rows, lanes = kv_ref.shape
    piece = gate_ref.shape[0]
    half = down_ref.shape[0] // 2
    last = pl.ds(rows - EXTRA, EXTRA)
    moves = [
        (gate_ref, a_ref.at[pl.ds(0, piece)]),
        (down_ref.at[pl.ds(0, half)], a_ref.at[pl.ds(piece, half)]),
        (value_ref, b_ref.at[pl.ds(0, piece)]),
        (down_ref.at[pl.ds(half, half)], b_ref.at[pl.ds(piece, half)]),
        (kv_ref.at[pl.ds(rows - HALO, HALO)], up_ref.at[pl.ds(0, HALO)]),
        (kv_ref.at[pl.ds(0, HALO)], dn_ref.at[pl.ds(0, HALO)]),
        (q_ref.at[last], up_ref.at[pl.ds(HALO, EXTRA)]),
        (q_ref.at[pl.ds(0, EXTRA)], dn_ref.at[pl.ds(HALO, EXTRA)]),
        (res_ref.at[last], edges.at[0]),
        (res_ref.at[pl.ds(0, EXTRA)], edges.at[1]),
    ]
    copies = [pltpu.make_async_copy(a, b, sems.at[j]) for j, (a, b) in enumerate(moves)]
    for c in copies:
        c.start()
    for c in copies:
        c.wait()
    full = edges.shape[2]
    for out, side, row in ((up_ref, 0, EXTRA - 1), (dn_ref, 1, 0)):
        out[HALO + EXTRA :] = jnp.concatenate(
            [edges[side, row : row + 1, lanes * j : lanes * (j + 1)] for j in range(full // lanes)], axis=0
        )


def prepare(q, kv, residual, gate, value, down_w):
    lanes = kv.shape[1]
    full = residual.shape[1]
    halo = ((HALO + EXTRA + full // lanes, lanes), BF16)
    stack = ((gate.shape[0] + down_w.shape[0] // 2, gate.shape[1]), BF16)
    return call(
        prepare_kernel,
        [halo, halo, stack, stack],
        tuple(pltpu.with_memory_space_constraint(x, pltpu.HBM) for x in (q, kv, residual, gate, value, down_w)),
        [ANY] * 6,
        4,
        [pltpu.VMEM((2, EXTRA, full), BF16), pltpu.SemaphoreType.DMA((10,))],
    )


def pair_kernel(a_ref, b_ref, out_ref):
    out_ref[0] = a_ref[...]
    out_ref[1] = b_ref[...]


def halves_kernel(in_ref, a_ref, b_ref):
    a_ref[...] = in_ref[0]
    b_ref[...] = in_ref[1]


def halves(x):
    return call(halves_kernel, [(x.shape[1:], BF16)] * 2, (x,), [VM], 4)


def pair(a, b):
    return call(pair_kernel, [((2, *a.shape), BF16)], (a, b), [VM, VM], 4)[0]


def pack_kernel(own, own_sw, far, far_sw, got, got_sw, g_ref, d_ref):
    piece = g_ref.shape[2]
    for c, ring in enumerate(
        ((own, got.at[0], got_sw.at[1], far), (own_sw, got.at[1], got_sw.at[0], far_sw))
    ):
        for i, ref in enumerate(ring):
            g_ref[c, i] = ref[0:piece]
            d_ref[c, i] = ref[piece:]


def pack(pieces, piece):
    rows, units = pieces[0].shape
    return call(pack_kernel, [((2, 4, piece, units), BF16), ((2, 4, rows - piece, units), BF16)], pieces, [VM] * 6, 6)


def document_row(docs_ref, index):
    count = docs_ref.shape[0]
    inside = ((index >= 0) & (index < count)).astype(jnp.int32)
    row = docs_ref[pl.ds(jnp.clip(index, 0, count - 1), 1), :]
    return (row * inside + (inside - 1)).astype(F32)


def column(row, n):
    return jnp.transpose(jnp.broadcast_to(row, (n, row.shape[1])))


def attention_kernel(sink_ref, q_ref, kv_ref, kl_ref, kr_ref, docs_ref, out_ref, kvx):
    rows = q_ref.shape[0]
    w = WINDOW
    width = 2 * HEAD_DIM
    blocks = rows // w
    kvx[0:HALO] = kl_ref[0:HALO]
    kvx[HALO : HALO + rows] = kv_ref[...]
    kvx[HALO + rows :] = kr_ref[0:HALO]
    base = lax.axis_index("sp") * blocks
    docs = {k: document_row(docs_ref, base + k) for k in range(-2, blocks + 2)}

    def heads(items):
        parts = []
        for q, keys, allowed in items:
            low = lax.broadcasted_iota(jnp.int32, q.shape, 1) < HEAD_DIM
            swapped = jnp.concatenate([q[:, HEAD_DIM:], q[:, :HEAD_DIM]], axis=1)
            zero = jnp.zeros_like(q)
            parts.append((jnp.where(low, q, zero), keys, allowed, sink_ref[0, 0]))
            parts.append((jnp.where(low, swapped, zero), keys, allowed, sink_ref[0, 1]))
        scores = [
            lax.dot_general(q, keys, LAST, preferred_element_type=F32) * HEAD_DIM**-0.5 for q, keys, _, _ in parts
        ]
        scores = [jnp.where(p[2], s, MASKED) for s, p in zip(scores, parts)]
        tops = [jnp.maximum(jnp.max(s, axis=-1, keepdims=True), p[3]) for s, p in zip(scores, parts)]
        exps = [jnp.exp(s - t) for s, t in zip(scores, tops)]
        totals = [jnp.sum(e, axis=-1, keepdims=True) + jnp.exp(p[3] - t) for e, t, p in zip(exps, tops, parts)]
        outs = [
            jnp.dot(e.astype(BF16), p[1], preferred_element_type=F32) * (1.0 / t)
            for e, t, p in zip(exps, totals, parts)
        ]
        results = []
        for j in range(len(items)):
            a, b = outs[2 * j], outs[2 * j + 1]
            low = lax.broadcasted_iota(jnp.int32, a.shape, 1) < HEAD_DIM
            first = jnp.concatenate([a[:, HEAD_DIM:], a[:, :HEAD_DIM]], axis=1)
            results.append(jnp.where(low, first, b).astype(BF16))
        return results

    away = lax.broadcasted_iota(jnp.int32, (w, 3 * w), 0) + w - lax.broadcasted_iota(jnp.int32, (w, 3 * w), 1)
    near = jnp.abs(away) <= WINDOW
    group = 4
    for first in range(0, blocks, group):
        items = []
        for i in range(first, first + group):
            own = jnp.concatenate([column(docs[i], w)] * 3, axis=1)
            allowed = near & (own == jnp.concatenate([docs[i - 1], docs[i], docs[i + 1]], axis=1))
            start = HALO - w + w * i
            items.append((q_ref[w * i : w * (i + 1)], kvx[start : start + 3 * w], allowed))
        for i, r in zip(range(first, first + group), heads(items)):
            out_ref[EXTRA + w * i : EXTRA + w * (i + 1)] = r

    span = 2 * HALO
    lead = 2 * w - HALO
    keys = jnp.concatenate([kvx[0:span], kvx[rows : rows + span]], axis=0)
    key_docs = jnp.concatenate(
        [
            jnp.concatenate([docs[k + j] for j in range(4)], axis=1)[:, lead : lead + span]
            for k in (-2, blocks - 2)
        ],
        axis=1,
    )
    row = lax.broadcasted_iota(jnp.int32, (EXTRA, 2 * span), 0)
    col = lax.broadcasted_iota(jnp.int32, (EXTRA, 2 * span), 1)
    key_at = jnp.where(col < span, col - HALO, col - span + rows - HALO)
    at = jnp.where(row == 0, rows, -1)
    own = jnp.where(row == 0, docs[blocks][:, 0:1], docs[-1][:, w - 1 : w])
    allowed = (jnp.abs(at - key_at) <= WINDOW) & (own == key_docs)
    qrow = lax.broadcasted_iota(jnp.int32, (EXTRA, width), 0)
    ahead = kr_ref[HALO : HALO + EXTRA].astype(F32)
    behind = kl_ref[HALO : HALO + EXTRA].astype(F32)
    qx = jnp.where(qrow == 0, ahead, behind).astype(BF16)
    outer = heads([(qx, keys, allowed)])[0]
    out_ref[0:EXTRA] = outer
    out_ref[EXTRA + rows :] = outer


def attend(q, kv, sink_logits, doc_table, left, right):
    rows, width = q.shape
    return call(
        attention_kernel,
        [((rows + 2 * EXTRA, width), BF16)],
        (sink_logits, q, kv, left, right, doc_table),
        [SM] + [VM] * 5,
        8,
        [pltpu.VMEM((rows + 2 * HALO, width), BF16)],
        flops=10**9,
    )[0]


def same_kernel(docs_ref, out_ref):
    w = docs_ref.shape[1]
    blocks = out_ref.shape[0] // w
    base = lax.axis_index("sp") * blocks
    lane = lax.broadcasted_iota(jnp.int32, (1, w), 1)
    docs = {k: document_row(docs_ref, base + k) for k in range(-1, blocks + 1)}
    for i in range(blocks):
        before = jnp.where(lane == 0, pltpu.roll(docs[i - 1], 1, 1), pltpu.roll(docs[i], 1, 1))
        after = jnp.where(lane == w - 1, pltpu.roll(docs[i + 1], w - 1, 1), pltpu.roll(docs[i], w - 1, 1))
        out_ref[w * i : w * (i + 1), 0:w] = column((before == docs[i]).astype(F32), w)
        out_ref[w * i : w * (i + 1), w : 2 * w] = column((after == docs[i]).astype(F32), w)


def project_kernel(*refs, blocks):
    single = lambda group: [r.at[i] for r in group[4:] for i in range(2)]
    att, weights = [list(g[:4]) + single(g) for g in (refs[:6], refs[6:12])]
    res_ref, left_ref, right_ref, gain_ref, normed_ref, mine_ref, wide, deep, stream, squares = refs[12:]
    rows, full = res_ref.shape
    lanes = left_ref.shape[1]
    part = mine_ref.shape[0]
    cols = 256
    for j in range(blocks):
        wide[:, lanes * j : lanes * (j + 1)] = att[j][...]
        deep[lanes * j : lanes * (j + 1)] = weights[j][...]
    squares[...] = jnp.zeros_like(squares)
    top = HALO + EXTRA
    row = lax.broadcasted_iota(jnp.int32, (EXTRA, cols), 0)
    for n in range(full // cols):
        proj = jnp.dot(wide[...], deep[:, cols * n : cols * (n + 1)], preferred_element_type=F32)
        j = top + n * (cols // lanes)
        ahead = jnp.concatenate([right_ref[j + i : j + i + 1] for i in range(cols // lanes)], axis=1).astype(F32)
        behind = jnp.concatenate([left_ref[j + i : j + i + 1] for i in range(cols // lanes)], axis=1).astype(F32)
        outer = jnp.where(row == 0, ahead, behind)
        for lo, hi, res in (
            (EXTRA, EXTRA + rows, res_ref[:, cols * n : cols * (n + 1)].astype(F32)),
            (0, EXTRA, outer),
            (EXTRA + rows, 2 * EXTRA + rows, outer),
        ):
            s = (res + proj[lo:hi]).astype(BF16)
            stream[lo:hi, cols * n : cols * (n + 1)] = s
            s = s.astype(F32)
            s = s * s
            squares[lo:hi] += s[:, :lanes] + s[:, lanes:]
    scale = lax.rsqrt(jnp.sum(squares[...], axis=-1, keepdims=True) * (1.0 / full) + EPSILON)
    squares[...] = jnp.broadcast_to(scale, squares.shape)
    tile = 352
    for t in range(0, rows + 2 * EXTRA, tile):
        for n in range(full // lanes):
            c = slice(lanes * n, lanes * (n + 1))
            normed_ref[t : t + tile, c] = (
                stream[t : t + tile, c].astype(F32) * squares[t : t + tile] * gain_ref[:, c]
            ).astype(BF16)
    mine_ref[...] = stream[pl.ds(pl.multiple_of(lax.axis_index("tp") * part + EXTRA, EXTRA), part), :]


def project(att, weights, residual, left, right, gain):
    rows, full = residual.shape
    all_rows = rows + 2 * EXTRA
    blocks = len(att) + 2
    lanes = att[0].shape[1]
    part = rows // lax.axis_size("tp")
    k = lanes * blocks
    return call(
        functools.partial(project_kernel, blocks=blocks),
        [((all_rows, full), BF16), ((part, full), BF16)],
        (*att, *weights, residual, left, right, gain),
        [VM] * 16,
        20,
        [
            pltpu.VMEM((all_rows, k), BF16),
            pltpu.VMEM((k, full), BF16),
            pltpu.VMEM((all_rows, full), BF16),
            pltpu.VMEM((all_rows, lanes), F32),
        ],
        flops=2 * all_rows * k * full,
    )


def place_pieces(refs, first_is_z, target, stride, shift, height):
    sp = lax.axis_index("sp")
    z, y = sp // NY, sp % NY
    up = 2 * (lax.axis_index("tp") % 2) - 1
    for slot, (ref, outer) in enumerate(zip(refs, (0, up, -up, 2))):
        for i, inner in enumerate((0, -up, up, 2) if slot == 2 else (0, up, -up, 2)):
            dz, dy = (inner, outer) if first_is_z else (outer, inner)
            block = (z + dz + NZ) % NZ * NY + (y + dy + NY) % NY
            at = pl.ds(pl.multiple_of(block * stride + shift, 16), height)
            target[at, :] = ref[0, i] if len(ref.shape) == 4 else ref[i]


def feed(block, normed_ref, same_ref, taps_ref, gw, vw, both, hidden_ref):
    rows, units = hidden_ref.shape
    lanes = 128
    start = block * rows
    wide = rows + 2 * EXTRA
    x = normed_ref[pl.ds(pl.multiple_of(start, rows), wide), :]
    same = pl.ds(pl.multiple_of(start, rows), rows)
    for n in range(units // lanes):
        cs = slice(lanes * n, lanes * (n + 1))
        slot = n % 2
        w = jnp.concatenate([gw[:, cs], vw[:, cs]], axis=1)
        r = jnp.dot(x, w, preferred_element_type=F32)
        both[slot, :, :lanes] = r[:, :lanes].astype(BF16).astype(F32)
        both[slot, :, lanes:] = r[:, lanes:]
        conved = (
            taps_ref[0:1, cs] * both[slot, EXTRA - 1 : EXTRA - 1 + rows, :lanes] * same_ref[same, :lanes]
            + taps_ref[1:2, cs] * both[slot, EXTRA : EXTRA + rows, :lanes]
            + taps_ref[2:3, cs] * both[slot, EXTRA + 1 : EXTRA + 1 + rows, :lanes] * same_ref[same, lanes:]
        )
        value = both[slot, EXTRA : EXTRA + rows, lanes:]
        hidden_ref[:, cs] = (jax.nn.gelu(conved, approximate=True) * value).astype(BF16)


def lower(hidden_ref, dw_ref, store):
    wide = 256
    for n in range(0, dw_ref.shape[0], wide):
        r = lax.dot_general(hidden_ref[...], dw_ref[n : n + wide, :], LAST, preferred_element_type=F32)
        store(slice(n, n + wide), r)


def position():
    tp = lax.axis_index("tp")
    return tp // 2, tp % 2


def by_core(core, r, part):
    low, high = r[:part], r[part:]
    mine = jnp.where(core == 0, low, high)
    return mine, jnp.where(core == 0, high, low)


def first_kernel(normed_ref, same_ref, taps_ref, *refs, nx):
    gw, vw, hidden_ref, both = refs[8:]
    piece = gw.shape[0] // (NZ * NY)
    place_pieces(refs[:4], True, gw, piece, 0, piece)
    place_pieces(refs[4:8], False, vw, piece, 0, piece)
    x, _ = position()
    feed(lax.rem(x + 2, nx), normed_ref, same_ref, taps_ref, gw, vw, both, hidden_ref)


def far_kernel(hidden_ref, *refs):
    dw_ref, send_ref, keep_ref = refs[8:]
    piece = dw_ref.shape[0] // (NZ * NY)
    half = piece // 2
    place_pieces(refs[:4], True, dw_ref, piece, 0, half)
    place_pieces(refs[4:8], False, dw_ref, piece, half, half)
    _, core = position()

    def store(at, r):
        keep, send = by_core(core, r, send_ref.shape[0])
        send_ref[:, at] = send.astype(BF16)
        keep_ref[:, at] = keep

    lower(hidden_ref, dw_ref, store)


def block_kernel(normed_ref, same_ref, taps_ref, gw, vw, dw_ref, *refs, which, nx):
    outs, both, hidden = refs[:-2], refs[-2], refs[-1]
    x, core = position()
    ahead = 1 - 2 * core
    step = {"other": -ahead, "near": ahead, "own": 0}[which]
    feed(lax.rem(x + step + nx, nx), normed_ref, same_ref, taps_ref, gw, vw, both, hidden)

    def store(at, r):
        if which == "own":
            keep, send = by_core(core, r, outs[0].shape[0])
            outs[0][:, at] = send.astype(BF16)
            outs[1][:, at] = keep
        else:
            outs[0][:, at] = r.astype(outs[0].dtype)

    lower(hidden, dw_ref, store)


def far_sum_kernel(keep_ref, got_ref, out_ref):
    out_ref[...] = (keep_ref[...] + got_ref[...].astype(F32)).astype(BF16)


def near_sum_kernel(keep_ref, got_ref, mine_ref, other_ref):
    _, core = position()
    wide = 256
    for n in range(0, keep_ref.shape[1], wide):
        at = slice(n, n + wide)
        mine, other = by_core(core, keep_ref[:, at] + got_ref[:, at].astype(F32), mine_ref.shape[0])
        mine_ref[:, at] = mine.astype(BF16)
        other_ref[:, at] = other.astype(BF16)


def add_kernel(a_ref, b_ref, out_ref):
    out_ref[...] = (a_ref[...].astype(F32) + b_ref[...].astype(F32)).astype(BF16)


def total_kernel(mine_ref, *refs):
    out_ref = refs[-1]
    s = mine_ref[...].astype(F32)
    for r in refs[:-1]:
        s = s + r[...].astype(F32)
    out_ref[...] = s.astype(BF16)


def on_device(
    queries,
    keys_values,
    sink_logits,
    doc_ids,
    residual,
    out_weight,
    ffn_gain,
    gate_weight,
    value_weight,
    conv_taps,
    down_weight,
):
    nz, ny = NZ, NY
    rows, full = residual.shape
    ntp = lax.axis_size("tp")
    nx = ntp // 2
    sp_count = nz * ny
    q = queries.reshape(rows, -1)
    kv = keys_values.reshape(rows, -1)
    doc_table = doc_ids.reshape(-1, 128)
    piece = gate_weight.shape[0]


    o_swap = swap_cores(out_weight)
    halo_up, halo_down, stack_a, stack_b = prepare(q, kv, residual, gate_weight, value_weight, down_weight)

    def ring(stack, axis):
        shift = lambda x: grid_shift(x, 2 * (axis == "z"), 2 * (axis == "y"), nz, ny)
        far = shift(stack)
        other = swap_cores(stack)
        got = core_shift(pair(stack, other), axis, nz, ny, nx)
        far_sw = swap_cores(far)
        got_sw = swap_cores(got)
        return pack((stack, other, far, far_sw, got, got_sw), piece)

    def plane(block, axis):
        got = core_shift(block, axis, nz, ny, nx)
        own, other = halves(got)
        return [block, own, swap_cores(other), core_shift(own, axis, nz, ny, nx)]

    gate_block, down_block_a = ring(stack_a, "z")
    value_block, down_block_b = ring(stack_b, "y")

    o_got = core_shift(pair(out_weight, o_swap), "x", nz, ny, nx)
    o_far = core_shift(halves(o_got)[0], "x", nz, ny, nx)
    o = [out_weight, o_swap, o_far, swap_cores(o_far), o_got, swap_cores(o_got)]

    ring_up = [(i, (i + 1) % sp_count) for i in range(sp_count)]
    ring_down = [((i + 1) % sp_count, i) for i in range(sp_count)]
    left = lax.ppermute(halo_up, "sp", ring_up)
    right = lax.ppermute(halo_down, "sp", ring_down)
    att = attend(q, kv, sink_logits, doc_table, left, right)
    t_far = tp_shift(att, 2, False, nx)
    t_swap = swap_cores(att)
    t_got = core_shift(pair(att, t_swap), "x", nz, ny, nx)
    t = [att, t_swap, t_far, swap_cores(t_far), t_got, swap_cores(t_got)]
    same = call(same_kernel, [((rows, 256), F32)], (doc_table,), [VM], 4)[0]

    gates = plane(gate_block, "y")
    values = plane(value_block, "z")
    downs_a = plane(down_block_a, "y")
    downs_b = plane(down_block_b, "z")
    normed, mine = project(t, o, residual, left, right, ffn_gain[None])

    units = conv_taps.shape[1]
    part = mine.shape[0]
    wide = 2 * part
    scratch = [pltpu.VMEM((2, wide + 2 * EXTRA, 256), F32), pltpu.VMEM((wide, units), BF16)]
    feed_flops = 4 * wide * full * units
    gw, vw, hidden = call(
        functools.partial(first_kernel, nx=nx),
        [((full, units), BF16), ((full, units), BF16), ((wide, units), BF16)],
        (normed, same, conv_taps, *gates, *values),
        [VM] * 11,
        8,
        scratch[:1],
        feed_flops,
    )
    dw, far_send, far_keep = call(
        far_kernel,
        [((full, units), BF16), ((part, full), BF16), ((part, full), F32)],
        (hidden, *downs_a, *downs_b),
        [VM] * 9,
        6,
        (),
        2 * wide * full * units,
    )

    def block(which, out):
        return call(
            functools.partial(block_kernel, which=which, nx=nx),
            out,
            (normed, same, conv_taps, gw, vw, dw),
            [VM] * 6,
            8,
            scratch,
            feed_flops,
        )

    simple = lambda kernel, out, args: call(kernel, out, args, [VM] * len(args), 6)
    small = ((part, full), BF16)
    far_got = swap_cores(far_send)
    (other_send,) = block("other", [((wide, full), BF16)])
    near_got = swap_cores(other_send)
    (far_sum,) = simple(far_sum_kernel, [small], (far_keep, far_got))
    far_came = core_shift(far_sum, "x", nz, ny, nx)
    (near_keep,) = block("near", [((wide, full), F32)])
    near_mine, near_other = simple(near_sum_kernel, [small, small], (near_keep, near_got))
    other_came = core_shift(near_other, "x", nz, ny, nx)
    own_send, own_keep = block("own", [small, ((part, full), F32)])
    own_got = swap_cores(own_send)
    (near_total,) = simple(add_kernel, [small], (near_mine, far_came))
    mine_came = core_shift(near_total, "x", nz, ny, nx)
    across = swap_cores(other_came)
    return simple(total_kernel, [small], (mine, own_keep, own_got, across, mine_came))[0]


def solution(mesh):
    in_specs = (
        P("sp", "tp", None),
        P("sp", "tp", None),
        P("tp", None),
        P(),
        P("sp", None),
        P("tp", None),
        P(),
        P("sp", "tp"),
        P("sp", "tp"),
        P(None, "tp"),
        P("sp", "tp"),
    )
    out_specs = P(("sp", "tp"), None)

    return jax.shard_map(on_device, mesh=mesh, in_specs=in_specs, out_specs=out_specs, check_vma=False)
```
